32 devices in a mesh: sp: 8 (over z, y), tp: 4 (over x, core).
Axes of the slice: x: 2, y: 2, z: 4, core: 2. Of those that a mesh axis runs over, the one named last changes fastest.
Arguments:
- query_rows: bfloat16 [4096, 2048], P('sp', 'tp'), may hold values from -40 to 40
- key_rows: bfloat16 [4096, 256], P('sp', 'tp'), may hold values from -6 to 6
- value_rows: bfloat16 [4096, 256], P('sp', 'tp'), may hold values from -12 to 12
- doc_ids: int32 [4096], P('sp'), may hold values from 0 to 3, never falling along the last dimension, each value on 1 to 2048 neighbouring positions
- sink_logit: float32 [32], P('tp'), may hold values from 1 to 6
- residual: bfloat16 [4096, 2048], P('sp'), may hold values from -10 to 10
- out_proj: bfloat16 [2048, 2048], P('tp'), may hold values from -0.25 to 0.25
- mix_gain: float32 [2048], replicated, may hold values from 0.1 to 1.9
- gate_proj: bfloat16 [2048, 5632], P('sp', 'tp'), may hold values from -0.125 to 0.125
- value_proj: bfloat16 [2048, 5632], P('sp', 'tp'), may hold values from -0.125 to 0.125
- gate_taps: float32 [3, 5632], P(None, 'tp'), may hold values from -3 to 3
- value_taps: float32 [3, 5632], P(None, 'tp'), may hold values from -3 to 3
- down_proj: bfloat16 [5632, 2048], P('tp', 'sp'), may hold values from -0.078125 to 0.078125
- final_gain: float32 [2048], P('tp'), may hold values from 0.1 to 1.9
Outputs:
- mixed: bfloat16 [4096, 2048], P('sp', 'tp')
The draws below stay inside these ranges and needn't reach their ends.
All inputs are finite; a program needn't handle non-finite values.
Results may differ from the reference program's by a relative error of at most 0.012.
Values may be sent and summed in bfloat16 or wider, within the bound.
A program may use at most 128 MiB of HBM per device.

```python
import math
import jax
import jax.numpy as jnp
import numpy as np
from jax import lax

D = 2048
HQ = 32
HK = 4
HD = 64
FF = 5632
WIN = 128
TAPS = 3
TOK_DEV = 512
TOKENS = 4096
DOC_COUNT = 4
DOC_MOST = 2048
N_TP = 4


def draw_key_rows(key, part):
    drawn = jax.random.truncated_normal(jax.random.fold_in(key, 1), -6.0, 6.0, (TOKENS, HK, HD), jnp.float32)
    return drawn.reshape(TOKENS, HK * HD).astype(jnp.bfloat16)


def draw_query_rows(key, part):
    drawn = jax.random.truncated_normal(jax.random.fold_in(key, 3), -6.0, 6.0, (TOKENS, HQ, HD), jnp.float32)
    return drawn.reshape(TOKENS, HQ * HD).astype(jnp.bfloat16)


def draw_residual(key, part):
    columns = jnp.arange(D, dtype=jnp.float32) / max(D - 1, 1)
    base = 0.4 * jax.random.truncated_normal(key, -6.0, 6.0, (TOKENS, D), jnp.float32)
    scale = jnp.exp(columns * math.log(4.0))
    return (base * scale[None, :]).astype(jnp.bfloat16)


def levels(stream_key, shape, pieces, smallest, largest):
    level, own = 1.0, jax.random.fold_in(stream_key, 6)
    for position, shards_of in pieces:
        steps = jnp.exp(jax.random.uniform(jax.random.fold_in(own, position), (shards_of,), jnp.float32, smallest / len(pieces), largest / len(pieces)))
        level = level * jnp.repeat(steps, shape[position] // shards_of).reshape([-1 if axis == position else 1 for axis in range(len(shape))])
    return level


def split_up(number_of, total, reach, skew):
    loads = [(1 << 20) // math.isqrt(standing ** skew) + 1 for standing in range(2, number_of + 1)]
    rest, holding = total - reach - (number_of - 1), [1] * (number_of - 1)
    while rest > 0:
        candidates = [i for i in range(number_of - 1) if holding[i] < reach]
        whole, left = sum([loads[i] for i in candidates]), rest
        for i in candidates:
            extra = min(reach - holding[i], max(1, left * loads[i] // whole), rest)
            holding[i] = holding[i] + extra
            rest = rest - extra
    return np.array([reach] + holding)


def uneven_parts(stream_key, count, total, most, slope):
    if count == 2:
        one = jax.random.randint(stream_key, (), max(1, total - most), min(most, total - 1) + 1)
        return jnp.stack([one, total - one])
    tallies = jnp.asarray(split_up(count, total, most, slope), jnp.int32)
    couples = (count - 1) // 2
    source_of, receiver = tallies[1:1 + 2 * couples:2], tallies[2:2 + 2 * couples:2]
    slack = jnp.minimum(source_of - 1, most - receiver)
    moved = jax.random.randint(jax.random.fold_in(stream_key, 1), (couples,), 0, 1 << 20) % (slack + 1)
    tallies = tallies.at[1:1 + 2 * couples:2].set(source_of - moved).at[2:2 + 2 * couples:2].set(receiver + moved)
    return tallies[jax.random.permutation(jax.random.fold_in(stream_key, 2), count)]


def noise(key, dims, scale, limit, pieces=(), kind=jnp.bfloat16):
    result = scale * jax.random.normal(key, dims, jnp.float32)
    if pieces:
        result = result * levels(key, dims, pieces, -0.22, 0.18)
    return jnp.clip(result, -limit, limit).astype(kind)


def setup_inputs(seed: int = 0) -> dict:
    arg_keys = jax.random.split(jax.random.key(seed), 15)
    return {
        "query_rows": draw_query_rows(jax.random.fold_in(arg_keys[14], 71), 0),
        "key_rows": draw_key_rows(jax.random.fold_in(arg_keys[14], 71), 0),
        "value_rows": noise(arg_keys[2], (TOKENS, HK * HD), 2.0, 12.0, ((0, 8), (1, 4))),
        "doc_ids": jnp.searchsorted(jnp.cumsum(uneven_parts(arg_keys[3], DOC_COUNT, TOKENS, DOC_MOST, 2)), jnp.arange(TOKENS), side="right").astype(jnp.int32),
        "sink_logit": jnp.clip(1.0 + 5.0 * jax.random.uniform(arg_keys[4], (HQ,), jnp.float32) ** levels(arg_keys[4], (HQ,), ((0, 4),), -0.2, 0.2), 1.0, 6.0),
        "residual": draw_residual(jax.random.fold_in(arg_keys[14], 71), 0),
        "out_proj": noise(arg_keys[6], (HQ * HD, D), (HQ * HD // 4) ** -0.5, 0.25, ((0, 4),)),
        "mix_gain": jnp.clip(1.0 + 0.18 * jax.random.normal(arg_keys[7], (D,), jnp.float32), 0.1, 1.9),
        "gate_proj": noise(arg_keys[8], (D, FF), D ** -0.5, 0.125, ((0, 8), (1, 4))),
        "value_proj": noise(arg_keys[9], (D, FF), D ** -0.5, 0.125, ((0, 8), (1, 4))),
        "gate_taps": noise(arg_keys[10], (TAPS, FF), 0.6, 3.0, ((1, 4),), jnp.float32),
        "value_taps": noise(arg_keys[11], (TAPS, FF), 0.6, 3.0, ((1, 4),), jnp.float32),
        "down_proj": noise(arg_keys[12], (FF, D), FF ** -0.5, 0.078125, ((0, 4), (1, 8))),
        "final_gain": jnp.clip(1.0 + 0.18 * jax.random.normal(arg_keys[13], (D,), jnp.float32), 0.1, 1.9),
    }


mix_scale = math.sqrt(2.0)
norm_eps = 1e-05

def attend(query_block, key_block, value_block, query_pos, key_pos, query_doc, key_doc, sink):
    head_size = query_block.shape[-1]
    scores = jnp.einsum('qkgd,skd->kgqs', query_block.astype(jnp.float32), key_block.astype(jnp.float32)) * head_size ** (-0.5)
    diff = query_pos[:, None] - key_pos[None, :]
    valid = (diff >= 0) & (diff < WIN) & (query_doc[:, None] == key_doc[None, :]) & (key_pos[None, :] >= 0)
    scores = jnp.where(valid[None, None], scores, -1e+30)
    top = jnp.maximum(lax.optimization_barrier(jnp.max(scores, axis=-1, keepdims=True)), sink)
    weights = jnp.exp(scores - top)
    total = lax.optimization_barrier(jnp.sum(weights, axis=-1, keepdims=True)) + jnp.exp(sink - top)
    probs = (weights / total).astype(jnp.bfloat16)
    out = jnp.einsum('kgqs,skd->qkgd', probs.astype(jnp.float32), value_block.astype(jnp.float32))
    return out.astype(jnp.bfloat16)

def depthwise(tail, current, taps, tail_docs, docs):
    extended = jnp.concatenate([tail, current])
    ext_docs = jnp.concatenate([tail_docs, docs])
    lag_rows = tail.shape[0]
    count = current.shape[0]
    total = jnp.zeros(current.shape, jnp.float32)
    for lag in range(lag_rows + 1):
        start = lag_rows - lag
        same = (ext_docs[start:start + count] == docs)[:, None]
        rows = extended[start:start + count].astype(jnp.float32)
        total = total + taps[lag].astype(jnp.float32)[None, :] * jnp.where(same, rows, 0.0)
    return total

def layer_norm(values, gain):
    mean = lax.optimization_barrier(jnp.mean(values, axis=1, keepdims=True))
    var = lax.optimization_barrier(jnp.mean(jnp.square(values - mean), axis=1, keepdims=True))
    return (values - mean) * lax.rsqrt(var + norm_eps) * gain.astype(jnp.float32)[None, :]

def reference(query_rows, key_rows, value_rows, doc_ids, sink_logit, residual, out_proj, mix_gain, gate_proj, value_proj, gate_taps, value_taps, down_proj, final_gain):
    groups = HQ // HK
    block = min(512, TOK_DEV)
    count = TOKENS // block
    queries = query_rows.reshape(TOKENS, HK, groups, HD)
    pad_keys = jnp.concatenate([jnp.zeros((WIN, HK * HD), jnp.bfloat16), key_rows]).reshape(TOKENS + WIN, HK, HD)
    pad_values = jnp.concatenate([jnp.zeros((WIN, HK * HD), jnp.bfloat16), value_rows]).reshape(TOKENS + WIN, HK, HD)
    docs = doc_ids.astype(jnp.int32)
    pad_docs = jnp.concatenate([jnp.full((WIN,), -1, jnp.int32), docs])
    sink = sink_logit.astype(jnp.float32).reshape(HK, groups, 1, 1)

    def one_block(index):
        start = (index * block).astype(jnp.int32)
        query_block = lax.dynamic_slice_in_dim(queries, start, block, 0)
        key_block = lax.dynamic_slice_in_dim(pad_keys, start, block + WIN, 0)
        value_block = lax.dynamic_slice_in_dim(pad_values, start, block + WIN, 0)
        query_doc = lax.dynamic_slice_in_dim(docs, start, block, 0)
        key_doc = lax.dynamic_slice_in_dim(pad_docs, start, block + WIN, 0)
        query_pos = start + jnp.arange(block, dtype=jnp.int32)
        key_pos = start - WIN + jnp.arange(block + WIN, dtype=jnp.int32)
        return attend(query_block, key_block, value_block, query_pos, key_pos, query_doc, key_doc, sink)
    heads = lax.map(one_block, jnp.arange(count, dtype=jnp.int32)).reshape(TOKENS, HQ * HD)
    head_cols = HQ * HD // N_TP
    attn_proj = jnp.zeros((TOKENS, D), jnp.float32)
    for group in range(N_TP):
        part = jnp.dot(heads[:, group * head_cols:(group + 1) * head_cols], out_proj[group * head_cols:(group + 1) * head_cols], preferred_element_type=jnp.float32)
        attn_proj = attn_proj + part.astype(jnp.bfloat16).astype(jnp.float32)
    first_sum = mix_scale * residual.astype(jnp.float32) + attn_proj
    normed = layer_norm(first_sum, mix_gain).astype(jnp.bfloat16)
    up_gate = jnp.dot(normed, gate_proj, preferred_element_type=jnp.float32).astype(jnp.bfloat16)
    up_value = jnp.dot(normed, value_proj, preferred_element_type=jnp.float32).astype(jnp.bfloat16)
    lag_rows = TAPS - 1
    zero_tail = jnp.zeros((lag_rows, FF), jnp.bfloat16)
    tail_docs = jnp.full((lag_rows,), -1, jnp.int32)
    conv_gate = depthwise(zero_tail, up_gate, gate_taps, tail_docs, docs)
    conv_value = depthwise(zero_tail, up_value, value_taps, tail_docs, docs)
    hidden = (jax.nn.gelu(conv_gate) * conv_value).astype(jnp.bfloat16)
    unit_cols = FF // N_TP
    ffn = jnp.zeros((TOKENS, D), jnp.float32)
    for group in range(N_TP):
        part = jnp.dot(hidden[:, group * unit_cols:(group + 1) * unit_cols], down_proj[group * unit_cols:(group + 1) * unit_cols], preferred_element_type=jnp.float32)
        ffn = ffn + part.astype(jnp.bfloat16).astype(jnp.float32)
    second_sum = mix_scale * normed.astype(jnp.float32) + ffn
    return layer_norm(second_sum, final_gain).astype(jnp.bfloat16)
```

```python
import functools
import math

import jax
import jax.numpy as jnp
from jax import lax
from jax.experimental import pallas as pl
from jax.experimental.pallas import tpu as pltpu
from jax.sharding import PartitionSpec as P

HD = 64
WIN = 128
TAPS = 3


mix_scale = math.sqrt(2.0)
norm_eps = 1e-05


def passed_along(block, axis, distance):
    devices = range(lax.axis_size(axis))
    route = [(i - distance, i) for i in devices if i - distance in devices]
    return lax.ppermute(block, axis, route)


def attend(query_block, key_block, value_block, query_pos, key_pos, query_doc, key_doc, sink):
    head_size = query_block.shape[-1]
    scores = jnp.einsum(
        "qkgd,skd->kgqs", query_block, key_block, preferred_element_type=jnp.float32
    ) * head_size ** (-0.5)
    diff = query_pos[:, None] - key_pos[None, :]
    valid = (
        (diff >= 0)
        & (diff < WIN)
        & (query_doc[:, None] == key_doc[None, :])
        & (key_pos[None, :] >= 0)
    )
    scores = jnp.where(valid[None, None], scores, -1e30)
    top = jnp.maximum(jnp.max(scores, axis=-1, keepdims=True), sink)
    weights = jnp.exp(scores - top)
    total = jnp.sum(weights, axis=-1, keepdims=True) + jnp.exp(sink - top)
    probs = (weights / total).astype(jnp.bfloat16)
    out = jnp.einsum("kgqs,skd->qkgd", probs, value_block, preferred_element_type=jnp.float32)
    return out.astype(jnp.bfloat16)


def depthwise(tail, current, taps, tail_docs, docs):
    extended = jnp.concatenate([tail, current])
    ext_docs = jnp.concatenate([tail_docs, docs])
    lag_rows = tail.shape[0]
    count = current.shape[0]
    total = jnp.zeros(current.shape, jnp.float32)
    for lag in range(lag_rows + 1):
        start = lag_rows - lag
        same = (ext_docs[start : start + count] == docs)[:, None]
        rows = extended[start : start + count].astype(jnp.float32)
        total = total + taps[lag][None, :] * jnp.where(same, rows, 0.0)
    return total


def on_device(
    query_rows,
    key_rows,
    value_rows,
    doc_ids,
    sink_logit,
    residual,
    out_proj,
    mix_gain,
    gate_proj,
    value_proj,
    gate_taps,
    value_taps,
    down_proj,
    final_gain,
):
    rows = query_rows.shape[0]
    kv_local = key_rows.shape[1] // HD
    heads_local = query_rows.shape[1] // HD
    groups = heads_local // kv_local
    offset = lax.axis_index("sp") * rows
    prev_keys, prev_values, prev_docs = passed_along(
        (key_rows[rows - WIN :], value_rows[rows - WIN :], doc_ids[rows - WIN :]), "sp", 1
    )
    all_keys = jnp.concatenate([prev_keys, key_rows]).reshape(rows + WIN, kv_local, HD)
    all_values = jnp.concatenate([prev_values, value_rows]).reshape(rows + WIN, kv_local, HD)
    all_docs = jnp.concatenate([prev_docs, doc_ids])
    key_pos = offset - WIN + jnp.arange(rows + WIN, dtype=jnp.int32)
    query_pos = offset + jnp.arange(rows, dtype=jnp.int32)
    queries = query_rows.reshape(rows, kv_local, groups, HD)
    sink = sink_logit.reshape(kv_local, groups, 1, 1)
    pieces = attend(queries, all_keys, all_values, query_pos, key_pos, doc_ids, all_docs, sink)
    heads = pieces.reshape(rows, heads_local * HD)
    partial_value = jnp.dot(heads, out_proj, preferred_element_type=jnp.float32)
    width = residual.shape[1]
    share = width // lax.axis_size("tp")
    col_start = lax.axis_index("tp") * share
    attn_total = lax.psum(partial_value.astype(jnp.bfloat16), "tp").astype(jnp.float32)
    first_sum = mix_scale * residual.astype(jnp.float32) + attn_total
    mean = jnp.mean(first_sum, axis=1, keepdims=True)
    var = jnp.mean(jnp.square(first_sum - mean), axis=1, keepdims=True)
    normed = ((first_sum - mean) * lax.rsqrt(var + norm_eps) * mix_gain[None, :]).astype(
        jnp.bfloat16
    )
    normed_own = lax.dynamic_slice_in_dim(normed, col_start, share, 1)
    up_gate = jnp.dot(
        normed,
        lax.all_gather(gate_proj, "sp", axis=0, tiled=True),
        preferred_element_type=jnp.float32,
    )
    up_value = jnp.dot(
        normed,
        lax.all_gather(value_proj, "sp", axis=0, tiled=True),
        preferred_element_type=jnp.float32,
    )
    up_gate = up_gate.astype(jnp.bfloat16)
    up_value = up_value.astype(jnp.bfloat16)
    lag_rows = TAPS - 1
    prev_gate, prev_value = passed_along(
        (up_gate[rows - lag_rows :], up_value[rows - lag_rows :]), "sp", 1
    )
    tail_docs = prev_docs[WIN - lag_rows :]
    conv_gate = depthwise(prev_gate, up_gate, gate_taps, tail_docs, doc_ids)
    conv_value = depthwise(prev_value, up_value, value_taps, tail_docs, doc_ids)
    hidden = (jax.nn.gelu(conv_gate) * conv_value).astype(jnp.bfloat16)
    terms = jnp.dot(
        hidden,
        lax.all_gather(down_proj, "sp", axis=1, tiled=True),
        preferred_element_type=jnp.float32,
    )
    ffn_own = lax.psum_scatter(
        terms.astype(jnp.bfloat16), "tp", scatter_dimension=1, tiled=True
    ).astype(jnp.float32)
    second_sum = mix_scale * normed_own.astype(jnp.float32) + ffn_own
    row_sum, row_squares = lax.psum(
        (jnp.sum(second_sum, axis=1), jnp.sum(second_sum * second_sum, axis=1)), "tp"
    )
    mean = row_sum / width
    var = row_squares / width - mean * mean
    return (
        (second_sum - mean[:, None]) * lax.rsqrt(var + norm_eps)[:, None] * final_gain[None, :]
    ).astype(jnp.bfloat16)


MESH = pl.DeviceIdType.MESH
LANES = 128
PAD = 16
F32 = jnp.float32
BF16 = jnp.bfloat16


def ring_index(position, count):
    position = lax.rem(position + 2 * count, count)
    return jnp.where(position < count // 2, 2 * position, 2 * (count - 1 - position) + 1)


def ring_position(index, count):
    return jnp.where(lax.rem(index, 2) == 0, index // 2, count - 1 - index // 2)


def layer_kernel(
    n,
    n_tp,
    kv_ref,
    docs_ref,
    sink_ref,
    query_ref,
    out_proj_ref,
    residual_ref,
    mix_ref,
    gate_ref,
    value_ref,
    gate_taps_ref,
    value_taps_ref,
    down_ref,
    final_ref,
    out_ref,
    gate_all,
    value_all,
    down_all,
    kv_ext,
    docs_ext,
    doc_cols,
    queries,
    proj,
    rest,
    heads,
    parts,
    parts_in,
    normed,
    up_gate,
    up_value,
    hidden,
    terms,
    terms_in,
    second,
    stats,
    ring_send,
    ring_recv,
    local_sem,
    halo_send,
    halo_recv,
    rows_send,
    rows_recv,
    norm_send,
    norm_recv,
    term_send,
    term_recv,
    stat_send,
    stat_recv,
):
    sp = lax.axis_index("sp")
    tp = lax.axis_index("tp")
    rows = query_ref.shape[0]
    ff = gate_ref.shape[1]
    width = residual_ref.shape[1]
    depth = gate_ref.shape[0]
    cols = down_ref.shape[1]
    share = width // n_tp
    per = share // cols
    steps = n // 2
    here = ring_position(sp, n)
    right = ring_index(here + 1, n)
    left = ring_index(here - 1, n)
    after = lax.rem(sp + 1, n)
    before = lax.rem(sp + n - 1, n)
    peers = [lax.rem(tp + i, n_tp) for i in range(1, n_tp)]

    barrier = pltpu.get_barrier_semaphore()
    for other in (right, left, after, before):
        pl.semaphore_signal(barrier, inc=1, device_id=(other, tp), device_id_type=MESH)
    for peer in peers:
        pl.semaphore_signal(barrier, inc=1, device_id=(sp, peer), device_id_type=MESH)
    pl.semaphore_wait(barrier, 4 + len(peers))

    whole = (gate_all, value_all, down_all)
    own = (gate_ref, value_ref, down_ref)
    half_rows = (depth // 2, depth // 2, ff // 2)

    def slot(w, index, half):
        size = half_rows[w]
        if w == 2:
            return down_all.at[index, pl.ds(half * size, size)]
        return whole[w].at[pl.ds(pl.multiple_of(index * depth + half * size, size), size)]

    def sending(w, way, step, half):
        if step == 1:
            source = own[w].at[pl.ds(half * half_rows[w], half_rows[w])]
            index = sp
        else:
            index = ring_index(here - (step - 1) if way == 0 else here + (step - 1), n)
            source = slot(w, index, half)
        return pltpu.make_async_remote_copy(
            src_ref=source,
            dst_ref=slot(w, index, half),
            send_sem=ring_send.at[w, way, step - 1, half],
            recv_sem=ring_recv.at[w, way, step - 1, half],
            device_id=(right if way == 0 else left, tp),
            device_id_type=MESH,
        )

    def arriving(w, way, step, half):
        index = ring_index(here - step if way == 0 else here + step, n)
        return pltpu.make_async_remote_copy(
            src_ref=slot(w, index, half),
            dst_ref=slot(w, index, half),
            send_sem=ring_send.at[w, way, step - 1, half],
            recv_sem=ring_recv.at[w, way, step - 1, half],
            device_id=(right if way == 0 else left, tp),
            device_id_type=MESH,
        )

    first_two = [
        (w, step, half) for step in range(1, steps) for w in (0, 1) for half in (0, 1)
    ] + [(0, steps, None), (1, steps, None)]
    last = [(2, step, half) for step in range(1, steps) for half in (0, 1)] + [(2, steps, None)]
    order = first_two + last
    early = len(first_two)

    def service(k):
        w, step, half = order[k]
        for way in (0, 1):
            part = way if half is None else half
            arriving(w, way, step, part).wait_recv()
            if step < steps - 1 or (step == steps - 1 and part == way):
                sending(w, way, step + 1, part).start()
        if k in (early - 4, early - 3):
            for way in (0, 1):
                sending(2, way, 1, k - (early - 4)).start()

    for w in (0, 1):
        for half in (0, 1):
            for way in (0, 1):
                sending(w, way, 1, half).start()

    halo = [
        pltpu.make_async_remote_copy(
            src_ref=kv_ref.at[pl.ds(rows - WIN, WIN)],
            dst_ref=kv_ext.at[pl.ds(0, WIN)],
            send_sem=halo_send.at[0],
            recv_sem=halo_recv.at[0],
            device_id=(after, tp),
            device_id_type=MESH,
        ),
        pltpu.make_async_remote_copy(
            src_ref=docs_ref.at[:, pl.ds(rows - WIN, WIN)],
            dst_ref=docs_ext.at[:, pl.ds(0, WIN)],
            send_sem=halo_send.at[1],
            recv_sem=halo_recv.at[1],
            device_id=(after, tp),
            device_id_type=MESH,
        ),
    ]
    for copy in halo:
        copy.start()
    row_share = rows // n_tp
    fetch = [
        pltpu.make_async_copy(kv_ref, kv_ext.at[pl.ds(WIN, rows)], local_sem.at[0]),
        pltpu.make_async_copy(docs_ref, docs_ext.at[:, pl.ds(WIN, rows)], local_sem.at[1]),
        pltpu.make_async_copy(query_ref, queries, local_sem.at[2]),
        pltpu.make_async_copy(out_proj_ref, proj, local_sem.at[3]),
        pltpu.make_async_copy(
            residual_ref.at[pl.ds(pl.multiple_of(tp * row_share, row_share), row_share)],
            rest,
            local_sem.at[4],
        ),
        pltpu.make_async_copy(
            gate_ref, gate_all.at[pl.ds(pl.multiple_of(sp * depth, depth), depth)], local_sem.at[5]
        ),
        pltpu.make_async_copy(
            value_ref, value_all.at[pl.ds(pl.multiple_of(sp * depth, depth), depth)], local_sem.at[6]
        ),
        pltpu.make_async_copy(down_ref, down_all.at[sp], local_sem.at[7]),
    ]
    for copy in fetch:
        copy.start()
    for copy in fetch:
        copy.wait()
    for copy in halo:
        copy.wait_recv()

    line = lax.broadcasted_iota(jnp.int32, (LANES, LANES), 0)
    lane = lax.broadcasted_iota(jnp.int32, (LANES, LANES), 1)
    for b in range(rows // LANES + 1):
        row = docs_ext[0:1, b * LANES : (b + 1) * LANES].astype(F32)
        doc_cols[b * LANES : (b + 1) * LANES, :] = jnp.broadcast_to(row, (LANES, LANES)).T

    low = lax.broadcasted_iota(jnp.int32, (2 * WIN, LANES), 1) < HD
    zero = jnp.zeros((2 * WIN, LANES), BF16)

    def attend_block(b, carry):
        start = pl.multiple_of(b * WIN, WIN)
        kv = kv_ext[pl.ds(start, 2 * WIN), 0:LANES]
        vk = kv_ext[pl.ds(start, 2 * WIN), LANES : 2 * LANES]
        keys = jnp.concatenate([jnp.where(low, kv, zero), jnp.where(low, zero, vk)], axis=0)
        values = jnp.concatenate([jnp.where(low, vk, zero), jnp.where(low, zero, kv)], axis=0)
        query_doc = doc_cols[pl.ds(start + WIN, WIN), :]
        prev_doc = docs_ext[0:1, pl.ds(start, WIN)].astype(F32)
        this_doc = docs_ext[0:1, pl.ds(start + WIN, WIN)].astype(F32)
        prev_ok = (query_doc == prev_doc) & (lane > line) & (sp * rows + b * WIN > 0)
        this_ok = (query_doc == this_doc) & (lane <= line)
        bias = jnp.concatenate(
            [jnp.where(prev_ok, 0.0, -1e30), jnp.where(this_ok, 0.0, -1e30)], axis=1
        ).astype(F32)
        for pair in range(query_ref.shape[1] // LANES):
            block = queries[pl.ds(start, WIN), pair * LANES : (pair + 1) * LANES]
            both = lax.dot_general(
                block, keys, (((1,), (1,)), ((), ())), preferred_element_type=F32
            )
            probs = []
            for side in (0, 1):
                scores = both[:, side * 2 * WIN : (side + 1) * 2 * WIN] * HD ** (-0.5) + bias
                sink = sink_ref[2 * pair + side]
                top = jnp.maximum(jnp.max(scores, axis=1, keepdims=True), sink)
                weights = jnp.exp(scores - top)
                total = jnp.sum(weights, axis=1, keepdims=True) + jnp.exp(sink - top)
                probs.append((weights / total).astype(BF16))
            heads[:, pair * LANES : (pair + 1) * LANES] = jnp.dot(
                jnp.concatenate(probs, axis=1), values, preferred_element_type=F32
            ).astype(BF16)
        for c in range(width // 512):
            parts[b, :, c * 512 : (c + 1) * 512] = jnp.dot(
                heads[...], proj[:, c * 512 : (c + 1) * 512], preferred_element_type=F32
            ).astype(BF16)

        for k in range(2):
            @pl.when(b == k + 1)
            def _():
                service(k)

        return carry

    lax.fori_loop(0, n_tp, attend_block, 0)
    done = 2

    def rows_copy(peer, source):
        return pltpu.make_async_remote_copy(
            src_ref=parts.at[peer],
            dst_ref=parts_in.at[source],
            send_sem=rows_send.at[peer],
            recv_sem=rows_recv.at[source],
            device_id=(sp, peer),
            device_id_type=MESH,
        )

    for peer in peers:
        rows_copy(peer, tp).start()
    for k in range(done, 5):
        service(k)
    done = 5
    for peer in peers:
        rows_copy(peer, peer).wait_recv()
    at = pl.multiple_of(PAD + tp * row_share, PAD)
    first = mix_scale * rest[...].astype(F32) + parts[tp].astype(F32)
    for peer in peers:
        first = first + parts_in[peer].astype(F32)
    mean = jnp.mean(first, axis=1, keepdims=True)
    first = first - mean
    var = jnp.mean(first * first, axis=1, keepdims=True)
    normed[pl.ds(at, row_share), :] = (first * lax.rsqrt(var + norm_eps) * mix_ref[...]).astype(
        BF16
    )

    service(done)
    done += 1

    def norm_copy(peer, source):
        place = pl.ds(pl.multiple_of(PAD + source * row_share, PAD), row_share)
        return pltpu.make_async_remote_copy(
            src_ref=normed.at[place],
            dst_ref=normed.at[place],
            send_sem=norm_send.at[peer],
            recv_sem=norm_recv.at[source],
            device_id=(sp, peer),
            device_id_type=MESH,
        )

    for peer in peers:
        norm_copy(peer, tp).start()
    for k in range(done, 9):
        service(k)
    done = 9
    for peer in peers:
        norm_copy(peer, peer).wait_recv()
    tail = pltpu.make_async_remote_copy(
        src_ref=normed.at[pl.ds(rows, PAD)],
        dst_ref=normed.at[pl.ds(0, PAD)],
        send_sem=halo_send.at[2],
        recv_sem=halo_recv.at[2],
        device_id=(after, tp),
        device_id_type=MESH,
    )
    tail.start()
    for k in range(done, early):
        service(k)
    tail.wait_recv()

    place = lax.broadcasted_iota(jnp.int32, (rows, LANES), 0) + sp * rows

    def convolved(source, taps_ref, at):
        total = taps_ref[0:1, pl.ds(at, LANES)] * source[PAD : PAD + rows, :]
        doc = doc_cols[WIN : WIN + rows, :]
        for lag in range(1, TAPS):
            same = (doc_cols[WIN - lag : WIN - lag + rows, :] == doc) & (place >= lag)
            shifted = jnp.where(same, source[PAD - lag : PAD - lag + rows, :], 0.0)
            total = total + taps_ref[lag : lag + 1, pl.ds(at, LANES)] * shifted
        return total

    def up_block(c, carry):
        at = pl.multiple_of(c * LANES, LANES)
        weights = jnp.concatenate(
            [gate_all[:, pl.ds(at, LANES)], value_all[:, pl.ds(at, LANES)]], axis=1
        )
        both = jnp.dot(normed[...], weights, preferred_element_type=F32)
        both = both.astype(BF16).astype(F32)
        up_gate[...] = both[:, :LANES]
        up_value[...] = both[:, LANES:]
        gate = convolved(up_gate, gate_taps_ref, at)
        value = convolved(up_value, value_taps_ref, at)
        inner = math.sqrt(2.0 / math.pi) * (gate + 0.044715 * (gate * gate * gate))
        hidden[:, pl.ds(at, LANES)] = (0.5 * gate * (1.0 + jnp.tanh(inner)) * value).astype(BF16)
        for k, when in ((0, 3), (1, 6), (2, 9)):
            @pl.when(c == when)
            def _():
                service(early + k)

        return carry

    lax.fori_loop(0, ff // LANES, up_block, 0)

    def term_copy(index, source):
        owner = index // per
        return pltpu.make_async_remote_copy(
            src_ref=terms.at[index],
            dst_ref=terms_in.at[source, lax.rem(index, per)],
            send_sem=term_send.at[index],
            recv_sem=term_recv.at[source, lax.rem(index, per)],
            device_id=(sp, owner),
            device_id_type=MESH,
        )

    def down_block(q, carry):
        for k in range(3, len(last)):
            @pl.when(q == 2 * (last[k][1] - 1) + 1)
            def _():
                service(early + k)

        distance = (q + 1) // 2
        index = ring_index(jnp.where(lax.rem(q, 2) == 1, here - distance, here + distance), n)
        terms[index] = jnp.dot(
            hidden[...], down_all[index], preferred_element_type=F32
        ).astype(BF16)

        @pl.when(index // per != tp)
        def _():
            term_copy(index, tp).start()

        return carry

    lax.fori_loop(0, n, down_block, 0)

    for peer in peers:
        for j in range(per):
            pltpu.make_async_remote_copy(
                src_ref=terms_in.at[peer, j],
                dst_ref=terms_in.at[peer, j],
                send_sem=term_send.at[0],
                recv_sem=term_recv.at[peer, j],
                device_id=(sp, peer),
                device_id_type=MESH,
            ).wait_recv()

    sums = jnp.zeros((rows, 1), F32)
    squares = jnp.zeros((rows, 1), F32)
    for j in range(per):
        mine = normed[PAD:, pl.ds(pl.multiple_of(tp * share + j * cols, cols), cols)]
        total = mix_scale * mine.astype(F32) + terms[tp * per + j].astype(F32)
        for peer in peers:
            total = total + terms_in[peer, j].astype(F32)
        second[:, j * cols : (j + 1) * cols] = total
        sums = sums + jnp.sum(total, axis=1, keepdims=True)
        squares = squares + jnp.sum(total * total, axis=1, keepdims=True)
    which = lax.broadcasted_iota(jnp.int32, (rows, LANES), 1)
    packed = jnp.where(which == 0, sums, jnp.where(which == 1, squares, 0.0))
    stats[tp] = packed.T[0:8]

    def stat_copy(peer, source):
        return pltpu.make_async_remote_copy(
            src_ref=stats.at[source],
            dst_ref=stats.at[source],
            send_sem=stat_send.at[peer],
            recv_sem=stat_recv.at[source],
            device_id=(sp, peer),
            device_id_type=MESH,
        )

    for peer in peers:
        stat_copy(peer, tp).start()
    for peer in peers:
        stat_copy(peer, peer).wait_recv()
    total = stats[0]
    for source in range(1, n_tp):
        total = total + stats[source]
    spread = jnp.concatenate([total] * (LANES // 8), axis=0).T
    mean = spread[:, 0:1] / width
    var = spread[:, 1:2] / width - mean * mean
    out_ref[...] = (
        (second[...] - mean) * lax.rsqrt(var + norm_eps) * final_ref[...]
    ).astype(BF16)

    for w in range(3):
        for way in (0, 1):
            for step in range(1, steps + 1):
                for half in (0, 1):
                    if step < steps or half == way:
                        sending(w, way, step, half).wait_send()
    for copy in halo:
        copy.wait_send()
    tail.wait_send()
    for peer in peers:
        rows_copy(peer, tp).wait_send()
        norm_copy(peer, tp).wait_send()
        stat_copy(peer, tp).wait_send()
        for j in range(per):
            term_copy(peer * per + j, tp).wait_send()


def fused(
    query_rows,
    key_rows,
    value_rows,
    doc_ids,
    sink_logit,
    residual,
    out_proj,
    mix_gain,
    gate_proj,
    value_proj,
    gate_taps,
    value_taps,
    down_proj,
    final_gain,
):
    n = lax.axis_size("sp")
    n_tp = lax.axis_size("tp")
    rows, head_cols = query_rows.shape
    width = residual.shape[1]
    depth, ff = gate_proj.shape
    cols = down_proj.shape[1]
    per = width // n_tp // cols
    steps = n // 2
    kv = jnp.concatenate([key_rows, value_rows, value_rows, key_rows], axis=1)
    docs = jnp.broadcast_to(doc_ids[None, :], (8, rows))
    share = rows // n_tp
    anywhere = pl.BlockSpec(memory_space=pl.ANY)
    vmem = pl.BlockSpec(memory_space=pltpu.VMEM)
    smem = pl.BlockSpec(memory_space=pltpu.SMEM)
    dma = pltpu.SemaphoreType.DMA
    return pl.pallas_call(
        functools.partial(layer_kernel, n, n_tp),
        out_shape=jax.ShapeDtypeStruct((rows, width // n_tp), BF16),
        in_specs=[
            anywhere, anywhere, smem, anywhere, anywhere, anywhere, vmem,
            anywhere, anywhere, vmem, vmem, anywhere, vmem,
        ],
        out_specs=vmem,
        scratch_shapes=[
            pltpu.VMEM((n * depth, ff), BF16),
            pltpu.VMEM((n * depth, ff), BF16),
            pltpu.VMEM((n, ff, cols), BF16),
            pltpu.VMEM((WIN + rows, 4 * HD), BF16),
            pltpu.VMEM((8, WIN + rows), jnp.int32),
            pltpu.VMEM((WIN + rows, LANES), F32),
            pltpu.VMEM((rows, head_cols), BF16),
            pltpu.VMEM((head_cols, width), BF16),
            pltpu.VMEM((share, width), BF16),
            pltpu.VMEM((share, head_cols), BF16),
            pltpu.VMEM((n_tp, share, width), BF16),
            pltpu.VMEM((n_tp, share, width), BF16),
            pltpu.VMEM((PAD + rows, width), BF16),
            pltpu.VMEM((PAD + rows, LANES), F32),
            pltpu.VMEM((PAD + rows, LANES), F32),
            pltpu.VMEM((rows, ff), BF16),
            pltpu.VMEM((n, rows, cols), BF16),
            pltpu.VMEM((n_tp, per, rows, cols), BF16),
            pltpu.VMEM((rows, width // n_tp), F32),
            pltpu.VMEM((n_tp, 8, rows), F32),
            dma((3, 2, steps, 2)),
            dma((3, 2, steps, 2)),
            dma((8,)),
            dma((3,)),
            dma((3,)),
            dma((n_tp,)),
            dma((n_tp,)),
            dma((n_tp,)),
            dma((n_tp,)),
            dma((n,)),
            dma((n_tp, per)),
            dma((n_tp,)),
            dma((n_tp,)),
        ],
        compiler_params=pltpu.CompilerParams(
            collective_id=0, has_side_effects=True, vmem_limit_bytes=60 * 1024 * 1024
        ),
        name="layer",
    )(
        kv,
        docs,
        sink_logit,
        query_rows,
        out_proj,
        residual,
        mix_gain[None, :],
        gate_proj,
        value_proj,
        gate_taps,
        value_taps,
        down_proj,
        final_gain[None, :],
    )


def on_any(*args):
    query_rows, key_rows, gate_proj, down_proj = args[0], args[1], args[8], args[12]
    n, n_tp = lax.axis_size("sp"), lax.axis_size("tp")
    share = args[5].shape[1] // n_tp
    depth, ff = gate_proj.shape
    cols = down_proj.shape[1]
    fits = (
        n % 2 == 0
        and n >= 8
        and ff >= 10 * LANES
        and query_rows.shape[0] == n_tp * WIN
        and key_rows.shape[1] == HD
        and query_rows.shape[1] % LANES == 0
        and depth % 32 == 0
        and ff % LANES == 0
        and cols % LANES == 0
        and share % cols == 0
    )
    return fused(*args) if fits else on_device(*args)


def solution(mesh):
    placed = (
        P("sp", "tp"),
        P("sp", "tp"),
        P("sp", "tp"),
        P("sp"),
        P("tp"),
        P("sp", None),
        P("tp", None),
        P(),
        P("sp", "tp"),
        P("sp", "tp"),
        P(None, "tp"),
        P(None, "tp"),
        P("tp", "sp"),
        P("tp"),
    )
    return jax.shard_map(
        on_any, mesh=mesh, in_specs=placed, out_specs=P("sp", "tp"), check_vma=False
    )
```

```python
import functools
import math

import jax
import jax.numpy as jnp
from jax import lax
from jax.experimental import pallas as pl
from jax.experimental.pallas import tpu as pltpu
from jax.sharding import PartitionSpec as P

HD = 64
WIN = 128
TAPS = 3


mix_scale = math.sqrt(2.0)
norm_eps = 1e-05


def passed_along(block, axis, distance):
    devices = range(lax.axis_size(axis))
    route = [(i - distance, i) for i in devices if i - distance in devices]
    return lax.ppermute(block, axis, route)


def attend(query_block, key_block, value_block, query_pos, key_pos, query_doc, key_doc, sink):
    head_size = query_block.shape[-1]
    scores = jnp.einsum(
        "qkgd,skd->kgqs", query_block, key_block, preferred_element_type=jnp.float32
    ) * head_size ** (-0.5)
    diff = query_pos[:, None] - key_pos[None, :]
    valid = (
        (diff >= 0)
        & (diff < WIN)
        & (query_doc[:, None] == key_doc[None, :])
        & (key_pos[None, :] >= 0)
    )
    scores = jnp.where(valid[None, None], scores, -1e30)
    top = jnp.maximum(jnp.max(scores, axis=-1, keepdims=True), sink)
    weights = jnp.exp(scores - top)
    total = jnp.sum(weights, axis=-1, keepdims=True) + jnp.exp(sink - top)
    probs = (weights / total).astype(jnp.bfloat16)
    out = jnp.einsum("kgqs,skd->qkgd", probs, value_block, preferred_element_type=jnp.float32)
    return out.astype(jnp.bfloat16)


def depthwise(tail, current, taps, tail_docs, docs):
    extended = jnp.concatenate([tail, current])
    ext_docs = jnp.concatenate([tail_docs, docs])
    lag_rows = tail.shape[0]
    count = current.shape[0]
    total = jnp.zeros(current.shape, jnp.float32)
    for lag in range(lag_rows + 1):
        start = lag_rows - lag
        same = (ext_docs[start : start + count] == docs)[:, None]
        rows = extended[start : start + count].astype(jnp.float32)
        total = total + taps[lag][None, :] * jnp.where(same, rows, 0.0)
    return total


def on_device(
    query_rows,
    key_rows,
    value_rows,
    doc_ids,
    sink_logit,
    residual,
    out_proj,
    mix_gain,
    gate_proj,
    value_proj,
    gate_taps,
    value_taps,
    down_proj,
    final_gain,
):
    rows = query_rows.shape[0]
    kv_local = key_rows.shape[1] // HD
    heads_local = query_rows.shape[1] // HD
    groups = heads_local // kv_local
    offset = lax.axis_index("sp") * rows
    prev_keys, prev_values, prev_docs = passed_along(
        (key_rows[rows - WIN :], value_rows[rows - WIN :], doc_ids[rows - WIN :]), "sp", 1
    )
    all_keys = jnp.concatenate([prev_keys, key_rows]).reshape(rows + WIN, kv_local, HD)
    all_values = jnp.concatenate([prev_values, value_rows]).reshape(rows + WIN, kv_local, HD)
    all_docs = jnp.concatenate([prev_docs, doc_ids])
    key_pos = offset - WIN + jnp.arange(rows + WIN, dtype=jnp.int32)
    query_pos = offset + jnp.arange(rows, dtype=jnp.int32)
    queries = query_rows.reshape(rows, kv_local, groups, HD)
    sink = sink_logit.reshape(kv_local, groups, 1, 1)
    pieces = attend(queries, all_keys, all_values, query_pos, key_pos, doc_ids, all_docs, sink)
    heads = pieces.reshape(rows, heads_local * HD)
    partial_value = jnp.dot(heads, out_proj, preferred_element_type=jnp.float32)
    width = residual.shape[1]
    share = width // lax.axis_size("tp")
    col_start = lax.axis_index("tp") * share
    attn_total = lax.psum(partial_value.astype(jnp.bfloat16), "tp").astype(jnp.float32)
    first_sum = mix_scale * residual.astype(jnp.float32) + attn_total
    mean = jnp.mean(first_sum, axis=1, keepdims=True)
    var = jnp.mean(jnp.square(first_sum - mean), axis=1, keepdims=True)
    normed = ((first_sum - mean) * lax.rsqrt(var + norm_eps) * mix_gain[None, :]).astype(
        jnp.bfloat16
    )
    normed_own = lax.dynamic_slice_in_dim(normed, col_start, share, 1)
    up_gate = jnp.dot(
        normed,
        lax.all_gather(gate_proj, "sp", axis=0, tiled=True),
        preferred_element_type=jnp.float32,
    )
    up_value = jnp.dot(
        normed,
        lax.all_gather(value_proj, "sp", axis=0, tiled=True),
        preferred_element_type=jnp.float32,
    )
    up_gate = up_gate.astype(jnp.bfloat16)
    up_value = up_value.astype(jnp.bfloat16)
    lag_rows = TAPS - 1
    prev_gate, prev_value = passed_along(
        (up_gate[rows - lag_rows :], up_value[rows - lag_rows :]), "sp", 1
    )
    tail_docs = prev_docs[WIN - lag_rows :]
    conv_gate = depthwise(prev_gate, up_gate, gate_taps, tail_docs, doc_ids)
    conv_value = depthwise(prev_value, up_value, value_taps, tail_docs, doc_ids)
    hidden = (jax.nn.gelu(conv_gate) * conv_value).astype(jnp.bfloat16)
    terms = jnp.dot(
        hidden,
        lax.all_gather(down_proj, "sp", axis=1, tiled=True),
        preferred_element_type=jnp.float32,
    )
    ffn_own = lax.psum_scatter(
        terms.astype(jnp.bfloat16), "tp", scatter_dimension=1, tiled=True
    ).astype(jnp.float32)
    second_sum = mix_scale * normed_own.astype(jnp.float32) + ffn_own
    row_sum, row_squares = lax.psum(
        (jnp.sum(second_sum, axis=1), jnp.sum(second_sum * second_sum, axis=1)), "tp"
    )
    mean = row_sum / width
    var = row_squares / width - mean * mean
    return (
        (second_sum - mean[:, None]) * lax.rsqrt(var + norm_eps)[:, None] * final_gain[None, :]
    ).astype(jnp.bfloat16)


MESH = pl.DeviceIdType.MESH
LANES = 128
PAD = 16
F32 = jnp.float32
BF16 = jnp.bfloat16


def layer_kernel(
    n,
    n_tp,
    kv_ref,
    docs_ref,
    sink_ref,
    query_ref,
    out_proj_ref,
    residual_ref,
    mix_ref,
    gate_ref,
    value_ref,
    gate_taps_ref,
    value_taps_ref,
    down_ref,
    final_ref,
    out_ref,
    gate_all,
    value_all,
    down_all,
    kv_ext,
    docs_ext,
    docs_other,
    doc_cols,
    work_cols,
    taps_gate,
    taps_value,
    queries,
    proj,
    rest,
    heads,
    parts,
    parts_in,
    norm_own,
    norm_cols,
    normed,
    up_gate,
    up_value,
    hidden,
    terms,
    terms_in,
    second,
    stats,
    plane_send,
    row_send,
    core_send,
    block_recv,
    local_sem,
    taps_send,
    taps_recv,
    halo_send,
    halo_recv,
    rows_send,
    rows_recv,
    norm_send,
    norm_recv,
    cols_send,
    cols_recv,
    tail_send,
    tail_recv,
    term_send,
    term_recv,
    stat_send,
    stat_recv,
):
    sp = lax.axis_index("sp")
    tp = lax.axis_index("tp")
    rows = query_ref.shape[0]
    ff = gate_ref.shape[1]
    width = residual_ref.shape[1]
    depth = gate_ref.shape[0]
    cols = down_ref.shape[1]
    share = width // n_tp
    per = share // cols
    planes = n // 2
    z, y = sp // 2, lax.rem(sp, 2)
    x, core = tp // 2, lax.rem(tp, 2)
    low = lax.rem(z, 2)
    home = low == core
    base = sp - 2 * low
    work = base + 2 * core
    unit = 2 * x + low
    partner = base + 2 * (1 - low)
    sibling = 2 * x + 1 - core
    across = 2 * z + 1 - y
    after = lax.rem(sp + 1, n)
    peers = [lax.rem(tp + i, n_tp) for i in range(1, n_tp)]
    everyone = n * n_tp
    me = sp * n_tp + tp

    barrier = pltpu.get_barrier_semaphore()

    def greet(i, carry):
        other = lax.rem(me + i, everyone)
        pl.semaphore_signal(
            barrier,
            inc=1,
            device_id=(other // n_tp, lax.rem(other, n_tp)),
            device_id_type=MESH,
        )
        return carry

    lax.fori_loop(1, everyone, greet, 0)
    pl.semaphore_wait(barrier, everyone - 1)

    whole = (gate_all, value_all, down_all)
    own = (gate_ref, value_ref, down_ref)

    def slot(w, index):
        if w == 2:
            return down_all.at[index]
        return whole[w].at[pl.ds(pl.multiple_of(index * depth, depth), depth)]

    def to_plane(w, i):
        return pltpu.make_async_remote_copy(
            src_ref=own[w],
            dst_ref=slot(w, sp),
            send_sem=plane_send.at[w, i],
            recv_sem=block_recv.at[w, sp],
            device_id=(2 * (core + 2 * i) + y, tp),
            device_id_type=MESH,
        )

    def forward(w, index, source, sems, where, device):
        return pltpu.make_async_remote_copy(
            src_ref=source,
            dst_ref=slot(w, index),
            send_sem=sems.at[w, where],
            recv_sem=block_recv.at[w, index],
            device_id=device,
            device_id_type=MESH,
        )

    def to_row(w, at, source):
        return forward(w, 2 * at + y, source, row_send, at, (across, tp))

    def to_core(w, index, source):
        return forward(w, index, source, core_send, index, (sp, sibling))

    def await_block(w, index):
        to_core(w, index, slot(w, index)).wait_recv()

    def pass_own(w):
        to_row(w, z, own[w]).start()
        to_core(w, sp, own[w]).start()

    def service(kind, w, j):
        at = lax.rem(z + j, planes)

        @pl.when(home)
        def _():
            if kind == "own":
                pass_own(w)
            elif kind == "col":
                await_block(w, 2 * at + y)
                to_row(w, at, slot(w, 2 * at + y)).start()
                to_core(w, 2 * at + y, slot(w, 2 * at + y)).start()
            else:
                await_block(w, 2 * at + 1 - y)
                to_core(w, 2 * at + 1 - y, slot(w, 2 * at + 1 - y)).start()

    def plane_step(w):
        for i in range(planes // 2):
            @pl.when(core + 2 * i != z)
            def _():
                if w > 0:
                    to_plane(w - 1, i).wait_send()
                if w < 3:
                    to_plane(w, i).start()

    plane_step(0)
    service("own", 0, 0)
    service("own", 1, 0)

    halo = [
        pltpu.make_async_remote_copy(
            src_ref=kv_ref.at[pl.ds(rows - WIN, WIN)],
            dst_ref=kv_ext.at[pl.ds(0, WIN)],
            send_sem=halo_send.at[0],
            recv_sem=halo_recv.at[0],
            device_id=(after, tp),
            device_id_type=MESH,
        ),
        pltpu.make_async_remote_copy(
            src_ref=docs_ref.at[:, pl.ds(rows - WIN, WIN)],
            dst_ref=docs_ext.at[:, pl.ds(0, WIN)],
            send_sem=halo_send.at[1],
            recv_sem=halo_recv.at[1],
            device_id=(after, tp),
            device_id_type=MESH,
        ),
    ]
    for copy in halo:
        copy.start()
    row_share = rows // n_tp
    fetch = [
        pltpu.make_async_copy(kv_ref, kv_ext.at[pl.ds(WIN, rows)], local_sem.at[0]),
        pltpu.make_async_copy(docs_ref, docs_ext.at[:, pl.ds(WIN, rows)], local_sem.at[1]),
        pltpu.make_async_copy(query_ref, queries, local_sem.at[2]),
        pltpu.make_async_copy(out_proj_ref, proj, local_sem.at[3]),
        pltpu.make_async_copy(
            residual_ref.at[pl.ds(pl.multiple_of(tp * row_share, row_share), row_share)],
            rest,
            local_sem.at[4],
        ),
    ]
    for copy in fetch:
        copy.start()
    settle = [pltpu.make_async_copy(own[w], slot(w, sp), local_sem.at[5 + w]) for w in range(3)]
    settle.append(pltpu.make_async_copy(gate_taps_ref, taps_gate, local_sem.at[8]))
    settle.append(pltpu.make_async_copy(value_taps_ref, taps_value, local_sem.at[9]))
    taps = [
        pltpu.make_async_remote_copy(
            src_ref=source,
            dst_ref=target,
            send_sem=taps_send.at[i],
            recv_sem=taps_recv.at[i],
            device_id=(sp, sibling),
            device_id_type=MESH,
        )
        for i, (source, target) in enumerate(
            ((gate_taps_ref, taps_gate), (value_taps_ref, taps_value))
        )
    ]

    @pl.when(home)
    def _():
        for copy in settle + taps:
            copy.start()

    for copy in fetch:
        copy.wait()
    for copy in halo:
        copy.wait_recv()
    docs_copy = pltpu.make_async_remote_copy(
        src_ref=docs_ext,
        dst_ref=docs_other,
        send_sem=halo_send.at[2],
        recv_sem=halo_recv.at[2],
        device_id=(partner, tp),
        device_id_type=MESH,
    )
    docs_copy.start()

    line = lax.broadcasted_iota(jnp.int32, (LANES, LANES), 0)
    lane = lax.broadcasted_iota(jnp.int32, (LANES, LANES), 1)
    for b in range(rows // LANES + 1):
        row = docs_ext[0:1, b * LANES : (b + 1) * LANES].astype(F32)
        doc_cols[b * LANES : (b + 1) * LANES, :] = jnp.broadcast_to(row, (LANES, LANES)).T

    left = lax.broadcasted_iota(jnp.int32, (2 * WIN, LANES), 1) < HD
    zero = jnp.zeros((2 * WIN, LANES), BF16)

    def attend_block(b, carry):
        start = pl.multiple_of(b * WIN, WIN)
        kv = kv_ext[pl.ds(start, 2 * WIN), 0:LANES]
        vk = kv_ext[pl.ds(start, 2 * WIN), LANES : 2 * LANES]
        keys = jnp.concatenate([jnp.where(left, kv, zero), jnp.where(left, zero, vk)], axis=0)
        values = jnp.concatenate([jnp.where(left, vk, zero), jnp.where(left, zero, kv)], axis=0)
        query_doc = doc_cols[pl.ds(start + WIN, WIN), :]
        prev_doc = docs_ext[0:1, pl.ds(start, WIN)].astype(F32)
        this_doc = docs_ext[0:1, pl.ds(start + WIN, WIN)].astype(F32)
        prev_ok = (query_doc == prev_doc) & (lane > line) & (sp * rows + b * WIN > 0)
        this_ok = (query_doc == this_doc) & (lane <= line)
        bias = jnp.concatenate(
            [jnp.where(prev_ok, 0.0, -1e30), jnp.where(this_ok, 0.0, -1e30)], axis=1
        ).astype(F32)
        for pair in range(query_ref.shape[1] // LANES):
            block = queries[pl.ds(start, WIN), pair * LANES : (pair + 1) * LANES]
            both = lax.dot_general(
                block, keys, (((1,), (1,)), ((), ())), preferred_element_type=F32
            )
            probs = []
            for side in (0, 1):
                scores = both[:, side * 2 * WIN : (side + 1) * 2 * WIN] * HD ** (-0.5) + bias
                sink = sink_ref[2 * pair + side]
                top = jnp.maximum(jnp.max(scores, axis=1, keepdims=True), sink)
                weights = jnp.exp(scores - top)
                total = jnp.sum(weights, axis=1, keepdims=True) + jnp.exp(sink - top)
                probs.append((weights / total).astype(BF16))
            heads[:, pair * LANES : (pair + 1) * LANES] = jnp.dot(
                jnp.concatenate(probs, axis=1), values, preferred_element_type=F32
            ).astype(BF16)
        for c in range(width // 512):
            parts[b, :, c * 512 : (c + 1) * 512] = jnp.dot(
                heads[...], proj[:, c * 512 : (c + 1) * 512], preferred_element_type=F32
            ).astype(BF16)

        @pl.when(b == n_tp - 1)
        def _():
            plane_step(1)

        for j in range(1, planes):
            @pl.when(b == min(j, n_tp - 1))
            def _():
                service("col", 0, j)

        return carry

    lax.fori_loop(0, n_tp, attend_block, 0)

    def rows_copy(peer, source):
        return pltpu.make_async_remote_copy(
            src_ref=parts.at[peer],
            dst_ref=parts_in.at[source],
            send_sem=rows_send.at[peer],
            recv_sem=rows_recv.at[source],
            device_id=(sp, peer),
            device_id_type=MESH,
        )

    for peer in peers:
        rows_copy(peer, tp).start()
    for peer in peers:
        rows_copy(peer, peer).wait_recv()
    first = mix_scale * rest[...].astype(F32) + parts[tp].astype(F32)
    for peer in peers:
        first = first + parts_in[peer].astype(F32)
    mean = jnp.mean(first, axis=1, keepdims=True)
    first = first - mean
    var = jnp.mean(first * first, axis=1, keepdims=True)
    norm_own[...] = (first * lax.rsqrt(var + norm_eps) * mix_ref[...]).astype(BF16)

    def workers(block):
        parity = lax.rem(block // 2, 2)
        return [
            (block - 2 * parity + 2 * a, 2 * b + parity)
            for a in (0, 1)
            for b in range(n_tp // 2)
        ]

    def place_of(source):
        return pl.ds(pl.multiple_of(PAD + source * row_share, PAD), row_share)

    def norm_copy(i, device, source):
        return pltpu.make_async_remote_copy(
            src_ref=norm_own,
            dst_ref=normed.at[place_of(source)],
            send_sem=norm_send.at[i],
            recv_sem=norm_recv.at[source],
            device_id=device,
            device_id_type=MESH,
        )

    def is_me(device):
        return (device[0] == sp) & (device[1] == tp)

    def cols_copy(i, peer, source):
        rows_at = pl.ds(pl.multiple_of(source * row_share, row_share), row_share)
        return pltpu.make_async_remote_copy(
            src_ref=norm_own.at[:, pl.ds(pl.multiple_of(peer * share, share), share)],
            dst_ref=norm_cols.at[rows_at],
            send_sem=cols_send.at[i],
            recv_sem=cols_recv.at[source],
            device_id=(sp, peer),
            device_id_type=MESH,
        )

    def tail_copy(i, device):
        return pltpu.make_async_remote_copy(
            src_ref=norm_own.at[pl.ds(row_share - PAD, PAD)],
            dst_ref=normed.at[pl.ds(0, PAD)],
            send_sem=tail_send.at[i],
            recv_sem=tail_recv,
            device_id=device,
            device_id_type=MESH,
        )

    own_workers = workers(sp)
    next_workers = workers(after)
    for i, device in enumerate(own_workers):
        @pl.when(jnp.logical_not(is_me(device)))
        def _():
            norm_copy(i, device, tp).start()

    @pl.when(tp == n_tp - 1)
    def _():
        for i, device in enumerate(next_workers):
            tail_copy(i, device).start()

    for i, peer in enumerate(peers):
        cols_copy(i, peer, tp).start()
    service("col", 1, 1)
    plane_step(2)

    @pl.when(home)
    def _():
        normed[place_of(tp), :] = norm_own[...]

    norm_cols[pl.ds(pl.multiple_of(tp * row_share, row_share), row_share), :] = norm_own[
        :, pl.ds(pl.multiple_of(tp * share, share), share)
    ]
    for j in range(planes):
        service("row", 0, j)
    for j in range(2, planes):
        service("col", 1, j)
    service("own", 2, 0)
    for j in range(planes):
        service("row", 1, j)
    docs_copy.wait_recv()
    for b in range(rows // LANES + 1):
        part = slice(b * LANES, (b + 1) * LANES)
        row = jnp.where(home, docs_ext[0:1, part], docs_other[0:1, part]).astype(F32)
        work_cols[part, :] = jnp.broadcast_to(row, (LANES, LANES)).T

    for source in range(n_tp):
        @pl.when(jnp.logical_not(home & (tp == source)))
        def _():
            norm_copy(0, (sp, sibling), source).wait_recv()

    tail_copy(0, (sp, sibling)).wait_recv()

    @pl.when(home)
    def _():
        for copy in settle:
            copy.wait()

    @pl.when(jnp.logical_not(home))
    def _():
        for copy in taps:
            copy.wait_recv()
        for w in (0, 1):
            for index in range(n):
                await_block(w, index)

    place = lax.broadcasted_iota(jnp.int32, (rows, LANES), 0) + work * rows

    def convolved(source, taps_ref, at):
        total = taps_ref[0:1, pl.ds(at, LANES)] * source[PAD : PAD + rows, :]
        doc = work_cols[WIN : WIN + rows, :]
        for lag in range(1, TAPS):
            same = (work_cols[WIN - lag : WIN - lag + rows, :] == doc) & (place >= lag)
            shifted = jnp.where(same, source[PAD - lag : PAD - lag + rows, :], 0.0)
            total = total + taps_ref[lag : lag + 1, pl.ds(at, LANES)] * shifted
        return total

    def up_block(c, carry):
        at = pl.multiple_of(c * LANES, LANES)
        weights = jnp.concatenate(
            [gate_all[:, pl.ds(at, LANES)], value_all[:, pl.ds(at, LANES)]], axis=1
        )
        both = jnp.dot(normed[...], weights, preferred_element_type=F32)
        both = both.astype(BF16).astype(F32)
        up_gate[...] = both[:, :LANES]
        up_value[...] = both[:, LANES:]
        gate = convolved(up_gate, taps_gate, at)
        value = convolved(up_value, taps_value, at)
        inner = math.sqrt(2.0 / math.pi) * (gate + 0.044715 * (gate * gate * gate))
        hidden[:, pl.ds(at, LANES)] = (0.5 * gate * (1.0 + jnp.tanh(inner)) * value).astype(BF16)
        for j in range(1, planes):
            @pl.when(c == 3 * j - 2)
            def _():
                service("col", 2, j)

        for j in (0, 1):
            @pl.when(c == 6 + 2 * j)
            def _():
                service("row", 2, j)

        return carry

    lax.fori_loop(0, ff // LANES, up_block, 0)
    for j in range(2, planes):
        service("row", 2, j)

    @pl.when(jnp.logical_not(home))
    def _():
        for index in range(n):
            await_block(2, index)

    def term_copy(index, source):
        owner = index // per
        return pltpu.make_async_remote_copy(
            src_ref=terms.at[index],
            dst_ref=terms_in.at[source, lax.rem(index, per)],
            send_sem=term_send.at[index],
            recv_sem=term_recv.at[source, lax.rem(index, per)],
            device_id=(work, owner),
            device_id_type=MESH,
        )

    def down_block(q, carry):
        index = lax.rem(q + per * 2 * (1 - x), n)
        terms[index] = jnp.dot(
            hidden[...], down_all[index], preferred_element_type=F32
        ).astype(BF16)

        mine = home & (index // per == tp)

        @pl.when(mine)
        def _():
            terms_in[tp, lax.rem(index, per)] = terms[index]

        @pl.when(jnp.logical_not(mine))
        def _():
            term_copy(index, unit).start()

        return carry

    lax.fori_loop(0, n, down_block, 0)

    for source in range(n_tp):
        @pl.when(jnp.logical_not(home & (tp == source)))
        def _():
            for j in range(per):
                pltpu.make_async_remote_copy(
                    src_ref=terms_in.at[source, j],
                    dst_ref=terms_in.at[source, j],
                    send_sem=term_send.at[0],
                    recv_sem=term_recv.at[source, j],
                    device_id=(sp, sibling),
                    device_id_type=MESH,
                ).wait_recv()

    for i, peer in enumerate(peers):
        cols_copy(i, peer, peer).wait_recv()

    sums = jnp.zeros((rows, 1), F32)
    squares = jnp.zeros((rows, 1), F32)
    for j in range(per):
        total = mix_scale * norm_cols[:, j * cols : (j + 1) * cols].astype(F32)
        for source in range(n_tp):
            total = total + terms_in[source, j].astype(F32)
        second[:, j * cols : (j + 1) * cols] = total
        sums = sums + jnp.sum(total, axis=1, keepdims=True)
        squares = squares + jnp.sum(total * total, axis=1, keepdims=True)
    which = lax.broadcasted_iota(jnp.int32, (rows, LANES), 1)
    packed = jnp.where(which == 0, sums, jnp.where(which == 1, squares, 0.0))
    stats[tp] = packed.T[0:8]

    def stat_copy(peer, source):
        return pltpu.make_async_remote_copy(
            src_ref=stats.at[source],
            dst_ref=stats.at[source],
            send_sem=stat_send.at[peer],
            recv_sem=stat_recv.at[source],
            device_id=(sp, peer),
            device_id_type=MESH,
        )

    for peer in peers:
        stat_copy(peer, tp).start()
    for peer in peers:
        stat_copy(peer, peer).wait_recv()
    total = stats[0]
    for source in range(1, n_tp):
        total = total + stats[source]
    spread = jnp.concatenate([total] * (LANES // 8), axis=0).T
    mean = spread[:, 0:1] / width
    var = spread[:, 1:2] / width - mean * mean
    out_ref[...] = (
        (second[...] - mean) * lax.rsqrt(var + norm_eps) * final_ref[...]
    ).astype(BF16)

    plane_step(3)

    @pl.when(home)
    def _():
        for w in range(3):
            for at in range(planes):
                to_row(w, at, slot(w, sp)).wait_send()
            for index in range(n):
                to_core(w, index, slot(w, index)).wait_send()
        for copy in taps:
            copy.wait_send()

    for copy in halo:
        copy.wait_send()
    docs_copy.wait_send()
    for i, device in enumerate(own_workers):
        @pl.when(jnp.logical_not(is_me(device)))
        def _():
            norm_copy(i, device, tp).wait_send()

    @pl.when(tp == n_tp - 1)
    def _():
        for i, device in enumerate(next_workers):
            tail_copy(i, device).wait_send()

    for i, peer in enumerate(peers):
        rows_copy(peer, tp).wait_send()
        cols_copy(i, peer, tp).wait_send()
        stat_copy(peer, tp).wait_send()
    for index in range(n):
        @pl.when(jnp.logical_not(home & (tp == index // per)))
        def _():
            term_copy(index, unit).wait_send()


def fused(
    query_rows,
    key_rows,
    value_rows,
    doc_ids,
    sink_logit,
    residual,
    out_proj,
    mix_gain,
    gate_proj,
    value_proj,
    gate_taps,
    value_taps,
    down_proj,
    final_gain,
):
    n = lax.axis_size("sp")
    n_tp = lax.axis_size("tp")
    rows, head_cols = query_rows.shape
    width = residual.shape[1]
    depth, ff = gate_proj.shape
    cols = down_proj.shape[1]
    per = width // n_tp // cols
    planes = n // 2
    kv = jnp.concatenate([key_rows, value_rows, value_rows, key_rows], axis=1)
    docs = jnp.broadcast_to(doc_ids[None, :], (8, rows))
    share = rows // n_tp
    anywhere = pl.BlockSpec(memory_space=pl.ANY)
    vmem = pl.BlockSpec(memory_space=pltpu.VMEM)
    smem = pl.BlockSpec(memory_space=pltpu.SMEM)
    dma = pltpu.SemaphoreType.DMA
    return pl.pallas_call(
        functools.partial(layer_kernel, n, n_tp),
        out_shape=jax.ShapeDtypeStruct((rows, width // n_tp), BF16),
        in_specs=[
            anywhere, anywhere, smem, anywhere, anywhere, anywhere, vmem,
            anywhere, anywhere, anywhere, anywhere, anywhere, vmem,
        ],
        out_specs=vmem,
        scratch_shapes=[
            pltpu.VMEM((n * depth, ff), BF16),
            pltpu.VMEM((n * depth, ff), BF16),
            pltpu.VMEM((n, ff, cols), BF16),
            pltpu.VMEM((WIN + rows, 4 * HD), BF16),
            pltpu.VMEM((8, WIN + rows), jnp.int32),
            pltpu.VMEM((8, WIN + rows), jnp.int32),
            pltpu.VMEM((WIN + rows, LANES), F32),
            pltpu.VMEM((WIN + rows, LANES), F32),
            pltpu.VMEM(gate_taps.shape, F32),
            pltpu.VMEM(gate_taps.shape, F32),
            pltpu.VMEM((rows, head_cols), BF16),
            pltpu.VMEM((head_cols, width), BF16),
            pltpu.VMEM((share, width), BF16),
            pltpu.VMEM((share, head_cols), BF16),
            pltpu.VMEM((n_tp, share, width), BF16),
            pltpu.VMEM((n_tp, share, width), BF16),
            pltpu.VMEM((share, width), BF16),
            pltpu.VMEM((rows, width // n_tp), BF16),
            pltpu.VMEM((PAD + rows, width), BF16),
            pltpu.VMEM((PAD + rows, LANES), F32),
            pltpu.VMEM((PAD + rows, LANES), F32),
            pltpu.VMEM((rows, ff), BF16),
            pltpu.VMEM((n, rows, cols), BF16),
            pltpu.VMEM((n_tp, per, rows, cols), BF16),
            pltpu.VMEM((rows, width // n_tp), F32),
            pltpu.VMEM((n_tp, 8, rows), F32),
            dma((3, planes // 2)),
            dma((3, planes)),
            dma((3, n)),
            dma((3, n)),
            dma((10,)),
            dma((2,)),
            dma((2,)),
            dma((3,)),
            dma((3,)),
            dma((n_tp,)),
            dma((n_tp,)),
            dma((n_tp,)),
            dma((n_tp,)),
            dma((n_tp,)),
            dma((n_tp,)),
            dma((n_tp,)),
            dma(()),
            dma((n,)),
            dma((n_tp, per)),
            dma((n_tp,)),
            dma((n_tp,)),
        ],
        compiler_params=pltpu.CompilerParams(
            collective_id=0, has_side_effects=True, vmem_limit_bytes=60 * 1024 * 1024
        ),
        name="layer",
    )(
        kv,
        docs,
        sink_logit,
        query_rows,
        out_proj,
        residual,
        mix_gain[None, :],
        gate_proj,
        value_proj,
        gate_taps,
        value_taps,
        down_proj,
        final_gain[None, :],
    )


def on_any(*args):
    query_rows, key_rows, gate_proj, down_proj = args[0], args[1], args[8], args[12]
    n, n_tp = lax.axis_size("sp"), lax.axis_size("tp")
    share = args[5].shape[1] // n_tp
    depth, ff = gate_proj.shape
    cols = down_proj.shape[1]
    fits = (
        n % 4 == 0
        and n_tp == 4
        and n >= 8
        and n <= n_tp * 2
        and ff >= 10 * LANES
        and query_rows.shape[0] == n_tp * WIN
        and key_rows.shape[1] == HD
        and query_rows.shape[1] % LANES == 0
        and depth % 32 == 0
        and ff % LANES == 0
        and cols % LANES == 0
        and share % cols == 0
    )
    return fused(*args) if fits else on_device(*args)


def solution(mesh):
    placed = (
        P("sp", "tp"),
        P("sp", "tp"),
        P("sp", "tp"),
        P("sp"),
        P("tp"),
        P("sp", None),
        P("tp", None),
        P(),
        P("sp", "tp"),
        P("sp", "tp"),
        P(None, "tp"),
        P(None, "tp"),
        P("tp", "sp"),
        P("tp"),
    )
    return jax.shard_map(
        on_any, mesh=mesh, in_specs=placed, out_specs=P("sp", "tp"), check_vma=False
    )
```
